256 devices in a mesh: ep: 64 (over z, y, core), tp: 4 (over x).
Axes of the slice: x: 4, y: 4, z: 8, core: 2. Of those that a mesh axis runs over, the one named last changes fastest.
Arguments:
- queries: bfloat16 [65536, 512], P('ep', 'tp'), may hold values from -6 to 6
- keys: bfloat16 [65536, 512], P('ep', 'tp'), may hold values from -6 to 6
- values: bfloat16 [65536, 1024], P('ep', 'tp'), may hold values from -6 to 6
- decay_rate: float32 [8], P('tp'), may hold values from 4.577637e-06 to 0.0333333333, as said below
- ret_gain: float32 [1024], P('tp'), may hold values from 0.1 to 1.9
- w_out: bfloat16 [1024, 2048], P('tp'), may hold values from -0.1875 to 0.1875
- moe_in: bfloat16 [32768, 2048], P(('ep', 'tp')), may hold values from -6 to 6
- ffn_gain: float32 [2048], replicated, may hold values from 0.1 to 1.9
- routes: int32 [32768, 2], P(('ep', 'tp')), may hold values from 0 to 63, all different within a row; in each aligned block of 128 rows (0 to 127, 128 to 255, ...) at most 5 rows name the same one
- route_weight: float32 [32768, 2], P(('ep', 'tp')), may hold values from 0.2 to 1
- expert_gate: bfloat16 [64, 2048, 3072], P('ep', None, 'tp'), may hold values from -0.125 to 0.125
- expert_up: bfloat16 [64, 2048, 3072], P('ep', None, 'tp'), may hold values from -0.125 to 0.125
- expert_down: bfloat16 [64, 3072, 2048], P('ep', 'tp'), may hold values from -0.109375 to 0.109375
Outputs:
- mix_out: bfloat16 [65536, 2048], P(('ep', 'tp'))
- moe_out: bfloat16 [32768, 2048], P(('ep', 'tp'))
The draws below stay inside these ranges and needn't reach their ends.
Inputs may be any that keep to these rules, and one draw needn't show every extreme that they name: `routes`: each row names 2 different experts. Among the 128 rows of one device no expert is named more than 5 times, and in every draw some device names some expert exactly 5 times. `decay_rate`: positive rates.
All inputs are finite; a program needn't handle non-finite values.
Results may differ from the reference program's by a relative error of at most 0.017.
Values may be sent and summed in bfloat16 or wider, within the bound.
No kernel may reach another device: no remote copies, remote signals or barrier semaphores. Data moves between devices by JAX's collectives and lax.ppermute only.
A program may use at most 128 MiB of HBM per device.

```python
import math
import jax
import jax.numpy as jnp
import numpy as np
from jax import lax

D = 2048
HEADS = 8
DK = 64
DV = 128
FF = 3072
TOP = 2
BLOCK = 128
MOE_DEV = 128
SEQ = 65536
MOE_TOKENS = 32768
EXPERTS = 64
CAP = 5
N_EP = 64
N_TP = 4


def draw_decay_rate(key, part):
    order = jax.random.permutation(jax.random.fold_in(key, 11), HEADS)
    slow = order < HEADS // 2
    slow_log = jax.random.uniform(jax.random.fold_in(key, 12), (HEADS,), jnp.float32, jnp.log(0.3 / SEQ), jnp.log(2.0 / SEQ))
    fast_log = jax.random.uniform(jax.random.fold_in(key, 13), (HEADS,), jnp.float32, jnp.log(1.0 / 100.0), jnp.log(1.0 / 30.0))
    return jnp.exp(jnp.where(slow, slow_log, fast_log)).astype(jnp.float32)


def levels(own_key, extent, split, smallest, largest):
    loudness, own = 1.0, jax.random.fold_in(own_key, 6)
    for dim, parts in split:
        steps = jnp.exp(jax.random.uniform(jax.random.fold_in(own, dim), (parts,), jnp.float32, smallest / len(split), largest / len(split)))
        loudness = loudness * jnp.repeat(steps, extent[dim] // parts).reshape([-1 if axis == dim else 1 for axis in range(len(extent))])
    return loudness


def deal_out(rng, own, number, rows, count, top, bound, slope):
    order = jax.random.permutation(rng, count)
    heavy_load, ordinary = portions_of(count, rows * top, bound, slope, True), portions_of(count, rows * top, bound, slope, False)
    places = jnp.arange(count)

    def named(tallies, rotation):
        used = int((tallies > 0).sum())
        fixed = max(1, used // 4)
        moved = fixed + (places - fixed + rotation * (used - fixed)) % max(1, count - fixed)
        return jnp.zeros((count,), jnp.int32).at[order[jnp.where(places < fixed, places, moved)]].set(jnp.asarray(tallies, jnp.int32))

    tallies = jnp.where(number % 4 == 0, named(heavy_load, number // 4), named(ordinary, number - number // 4 - 1))
    mixed = jax.random.permutation(jax.random.fold_in(own, 3), count)
    donor, taker = mixed[0:count // 2 * 2:2], mixed[1:count // 2 * 2:2]
    slack = jnp.minimum(tallies[donor] - 1, bound - tallies[taker]) // 2
    slack = jnp.where((donor == order[0]) | (taker == order[0]) | (tallies[taker] == 0), 0, jnp.maximum(slack, 0))
    moved = jax.random.randint(jax.random.fold_in(own, 4), (count // 2,), 0, 1 << 20) % (slack + 1)
    tallies = tallies.at[donor].add(-moved).at[taker].add(moved)
    labels = jnp.searchsorted(jnp.cumsum(tallies), jnp.arange(rows * top), side="right").astype(jnp.int32)
    table = labels.reshape(top, rows).T
    table = table[jax.random.permutation(jax.random.fold_in(own, 1), rows)]
    rotation = jax.random.randint(jax.random.fold_in(own, 2), (rows, 1), 0, top)
    return jnp.take_along_axis(table, (jnp.arange(top)[None, :] + rotation) % top, axis=1)


def portions_of(amount, total, bound, lean, full):
    loads = [(1 << 20) // math.isqrt(grade ** lean) + 1 for grade in range(1, amount + 1)]
    largest = bound if full else min(bound, max(-(-total // amount), total * loads[0] // sum(loads)))
    least = 1 if total - largest >= amount - 1 else 0
    holding, surplus = [largest] + [least] * (amount - 1), total - largest - least * (amount - 1)
    while surplus > 0:
        free = [i for i in range(1, amount) if holding[i] < largest] or [i for i in range(1, amount) if holding[i] < bound]
        whole, left = sum([loads[i] for i in free]), surplus
        for i in free:
            extra = min(bound - holding[i], max(1, left * loads[i] // whole), surplus)
            holding[i] = holding[i] + extra
            surplus = surplus - extra
    return np.array(holding)


def normal_values(stream_key, dims, scale, bound, cuts=(), kind=jnp.bfloat16):
    level = levels(stream_key, dims, cuts, -0.22, 0.18) if cuts else 1.0
    entries = jax.random.normal(stream_key, dims, jnp.float32) * scale * level
    return jnp.minimum(jnp.maximum(entries, -bound), bound).astype(kind)


def setup_inputs(seed: int = 0) -> dict:
    key_of = jax.random.split(jax.random.key(seed), 14)
    queries = normal_values(key_of[0], (SEQ, HEADS * DK), 1.0, 6.0, ((0, 64), (1, 4)))
    keys = normal_values(key_of[1], (SEQ, HEADS * DK), 1.0, 6.0, ((0, 64), (1, 4)))
    values = normal_values(key_of[2], (SEQ, HEADS * DV), 1.0, 6.0, ((0, 64), (1, 4)))
    decay_rate = draw_decay_rate(jax.random.fold_in(key_of[13], 71), 0)
    ret_gain = jnp.clip(1.0 + 0.18 * jax.random.normal(key_of[4], (HEADS * DV,), jnp.float32), 0.1, 1.9)
    w_out = normal_values(key_of[5], (HEADS * DV, D), (HEADS * DV) ** -0.5, 0.1875, ((0, 4),))
    moe_in = normal_values(key_of[6], (MOE_TOKENS, D), 1.0, 6.0, ((0, 256),))
    ffn_gain = jnp.clip(1.0 + 0.18 * jax.random.normal(key_of[7], (D,), jnp.float32), 0.1, 1.9)
    routes_keys = jax.random.split(jax.random.fold_in(key_of[8], 1), MOE_TOKENS // MOE_DEV)
    routes_turns = jax.random.permutation(jax.random.fold_in(key_of[8], 3), MOE_TOKENS // MOE_DEV)
    routes = jax.vmap(lambda own, number: deal_out(jax.random.fold_in(key_of[8], 2), own, number, MOE_DEV, EXPERTS, TOP, CAP, 1))(routes_keys, routes_turns).reshape((MOE_TOKENS, TOP))
    route_weight = jnp.clip(0.2 + 0.8 * jax.random.uniform(key_of[9], (MOE_TOKENS, TOP), jnp.float32) ** levels(key_of[9], (MOE_TOKENS, TOP), ((0, 256),), -0.2, 0.2), 0.2, 1.0)
    expert_gate = normal_values(key_of[10], (EXPERTS, D, FF), D ** -0.5, 0.125, ((0, 64), (2, 4)))
    expert_up = normal_values(key_of[11], (EXPERTS, D, FF), D ** -0.5, 0.125, ((0, 64), (2, 4)))
    expert_down = normal_values(key_of[12], (EXPERTS, FF, D), FF ** -0.5, 0.109375, ((0, 64), (1, 4)))
    return {"queries": queries, "keys": keys, "values": values, "decay_rate": decay_rate, "ret_gain": ret_gain, "w_out": w_out, "moe_in": moe_in, "ffn_gain": ffn_gain, "routes": routes, "route_weight": route_weight, "expert_gate": expert_gate, "expert_up": expert_up, "expert_down": expert_down}


EPS = 1e-06
ROPE_BASE = 10000.0
HIGH = lax.Precision.HIGHEST

def rotate(vectors, positions):
    half = vectors.shape[-1] // 2
    inv_freq = ROPE_BASE ** (-jnp.arange(half, dtype=jnp.float32) / half)
    angle = positions[:, None] * inv_freq[None, :]
    cosine = jnp.cos(angle)[:, None, :]
    sine = jnp.sin(angle)[:, None, :]
    first = vectors[..., :half]
    second = vectors[..., half:]
    return jnp.concatenate([first * cosine - second * sine, second * cosine + first * sine], axis=-1)

def retention_all(queries, keys, values, decay_rate):
    length = queries.shape[0]
    heads = decay_rate.shape[0]
    positions = jnp.arange(length, dtype=jnp.float32)
    q_rot = rotate(queries.astype(jnp.float32).reshape(length, heads, DK), positions) * DK ** (-0.5)
    k_rot = rotate(keys.astype(jnp.float32).reshape(length, heads, DK), positions)
    v_all = values.astype(jnp.float32).reshape(length, heads, DV)
    blocks = length // BLOCK
    q_blk = q_rot.reshape(blocks, BLOCK, heads, DK).transpose(0, 2, 1, 3)
    k_blk = k_rot.reshape(blocks, BLOCK, heads, DK).transpose(0, 2, 1, 3)
    v_blk = v_all.reshape(blocks, BLOCK, heads, DV).transpose(0, 2, 1, 3)
    log_g = -decay_rate
    index = jnp.arange(BLOCK, dtype=jnp.float32)
    diff = index[:, None] - index[None, :]
    dmat = jnp.where(diff >= 0, jnp.exp(log_g[:, None, None] * jnp.maximum(diff, 0.0)), 0.0)
    k_decay = jnp.exp(log_g[:, None] * (BLOCK - 1.0 - index))
    q_decay = jnp.exp(log_g[:, None] * (index + 1.0))
    block_decay = jnp.exp(log_g * BLOCK)

    def step(state, inputs):
        q_now, k_now, v_now = inputs
        scores = jnp.einsum('hid,hjd->hij', q_now, k_now, precision=HIGH) * dmat
        inner = jnp.einsum('hij,hje->hie', scores, v_now, precision=HIGH)
        cross = jnp.einsum('hid,hde->hie', q_now * q_decay[:, :, None], state, precision=HIGH)
        update = jnp.einsum('hjd,hje->hde', k_now * k_decay[:, :, None], v_now, precision=HIGH)
        return (state * block_decay[:, None, None] + update, inner + cross)
    start = jnp.zeros((heads, DK, DV), jnp.float32)
    _, outs = lax.scan(step, start, (q_blk, k_blk, v_blk))
    return outs.transpose(0, 2, 1, 3).reshape(length, heads, DV)

def slot_numbers(route_block, experts):
    flat = route_block.reshape(-1)
    hits = (flat[:, None] == jnp.arange(experts, dtype=jnp.int32)[None, :]).astype(jnp.int32)
    before = jnp.cumsum(hits, axis=0) - hits
    return lax.optimization_barrier(jnp.sum(before * hits, axis=1)).astype(jnp.int32).reshape(route_block.shape)

def reference(queries, keys, values, decay_rate, ret_gain, w_out, moe_in, ffn_gain, routes, route_weight, expert_gate, expert_up, expert_down):
    heads = decay_rate.shape[0]
    ret = retention_all(queries, keys, values, decay_rate)
    mean_sq = lax.optimization_barrier(jnp.mean(ret * ret, axis=-1, keepdims=True))
    normed_heads = ret * lax.rsqrt(mean_sq + EPS) * ret_gain.reshape(heads, DV)
    y_rows = normed_heads.reshape(ret.shape[0], heads * DV).astype(jnp.bfloat16)
    group = heads * DV // N_TP
    total = jnp.zeros((y_rows.shape[0], D), jnp.float32)
    for index in range(N_TP):
        part = jnp.dot(y_rows[:, index * group:(index + 1) * group], w_out[index * group:(index + 1) * group], preferred_element_type=jnp.float32)
        total = total + lax.optimization_barrier(part.astype(jnp.bfloat16)).astype(jnp.float32)
    mix_out = total.astype(jnp.bfloat16)
    sources = N_EP * N_TP
    x_float = moe_in.astype(jnp.float32)
    normed = (x_float * lax.rsqrt(lax.optimization_barrier(jnp.mean(x_float * x_float, axis=-1, keepdims=True)) + EPS) * ffn_gain).astype(jnp.bfloat16)
    route_blocks = routes.reshape(sources, MOE_DEV, TOP)
    slots = jax.vmap(lambda block: slot_numbers(block, EXPERTS))(route_blocks).reshape(-1, TOP)
    source = jnp.broadcast_to((jnp.arange(MOE_TOKENS, dtype=jnp.int32) // MOE_DEV)[:, None], routes.shape).astype(jnp.int32)
    spread_rows = jnp.broadcast_to(normed[:, None, :], (MOE_TOKENS, TOP, D))
    buffer = jnp.zeros((EXPERTS, sources, CAP, D), jnp.bfloat16).at[routes, source, slots].set(spread_rows)
    width = FF // N_TP

    def expert(inputs):
        rows, gate_w, up_w, down_w = inputs
        rows = rows.reshape(sources * CAP, D)
        gate = jnp.dot(rows, gate_w, preferred_element_type=jnp.float32)
        up = jnp.dot(rows, up_w, preferred_element_type=jnp.float32)
        hidden = (jax.nn.silu(gate) * up).astype(jnp.bfloat16)
        acc = jnp.zeros((sources * CAP, D), jnp.float32)
        for index in range(N_TP):
            part = jnp.dot(hidden[:, index * width:(index + 1) * width], down_w[index * width:(index + 1) * width], preferred_element_type=jnp.float32)
            acc = acc + lax.optimization_barrier(part.astype(jnp.bfloat16)).astype(jnp.float32)
        return acc.astype(jnp.bfloat16).reshape(sources, CAP, D)
    results = lax.map(expert, (buffer, expert_gate, expert_up, expert_down))
    picked = results[routes, source, slots]
    moe_out = lax.optimization_barrier(jnp.sum(route_weight[:, :, None] * picked.astype(jnp.float32), axis=1)).astype(jnp.bfloat16)
    return (mix_out, moe_out)
```

```python
import jax
import jax.numpy as jnp
from jax import lax
from jax.experimental import pallas as pl
from jax.experimental.pallas import tpu as pltpu
from jax.sharding import Mesh
from jax.sharding import PartitionSpec as P


DK = 64
DV = 128
LANES = 128
QBLOCK = 256
TILE = 256
EP = ("ep_0", "ep_1", "ep_2")
EP_TP = ("ep_0", "ep_1", "ep_2", "tp")
SLOTS = ((0, 2), (2, 3))

EPS = 1e-06
ROPE_BASE = 10000.0
F32 = jnp.float32
BF16 = jnp.bfloat16


def params(mib=14):
    return pltpu.CompilerParams(vmem_limit_bytes=mib * 1024 * 1024)


def cost(flops, num_bytes):
    return pl.CostEstimate(flops=int(flops), bytes_accessed=int(num_bytes), transcendentals=0)


def split(x):
    high = x.astype(BF16)
    return high, (x - high.astype(F32)).astype(BF16)


def product(a, b, dims):
    def dot(x, y):
        return lax.dot_general(x, y, (dims, ((), ())), preferred_element_type=F32)

    a_high, a_low = split(a)
    if b.dtype == BF16:
        return dot(a_high, b) + dot(a_low, b)
    b_high, b_low = split(b)
    return dot(a_high, b_high) + (dot(a_high, b_low) + dot(a_low, b_high))


PLAIN = ((1,), (0,))
RIGHT = ((1,), (1,))
LEFT = ((0,), (0,))


def place(x, gain, routes, experts, cap):
    rows, width = x.shape
    cuts = width // LANES
    lines = experts * cap

    def body(x_ref, g_ref, r_ref, o_ref, slot_ref, scr):
        xf = x_ref[...].astype(F32)
        normed = (
            xf * lax.rsqrt(jnp.mean(xf * xf, axis=-1, keepdims=True) + EPS) * g_ref[...]
        ).astype(BF16)
        r0 = r_ref[:, 0:1]
        r1 = r_ref[:, 1:2]
        ids = lax.broadcasted_iota(jnp.int32, (rows, experts), 1)
        h0 = r0 == ids
        h1 = r1 == ids
        hits = jnp.where(h0 | h1, 1.0, 0.0).astype(BF16)
        tri = jnp.where(
            lax.broadcasted_iota(jnp.int32, (rows, rows), 0)
            > lax.broadcasted_iota(jnp.int32, (rows, rows), 1),
            1.0,
            0.0,
        ).astype(BF16)
        before = jnp.dot(tri, hits, preferred_element_type=F32)
        s0 = jnp.sum(jnp.where(h0, before, 0.0), axis=1, keepdims=True).astype(jnp.int32)
        s1 = jnp.sum(jnp.where(h1, before, 0.0), axis=1, keepdims=True).astype(jnp.int32)
        slot_ref[:, 0:1] = s0
        slot_ref[:, 1:2] = s1
        col = lax.broadcasted_iota(jnp.int32, (rows, lines), 1)
        hot = (col == r0 * cap + s0) | (col == r1 * cap + s1)
        hot = jnp.where(hot, 1.0, 0.0).T.astype(BF16)
        moved = jnp.dot(hot, normed, preferred_element_type=F32)
        for c in range(cuts):
            scr[pl.ds(c, lines, stride=cuts), :] = moved[:, c * LANES : (c + 1) * LANES]
        o_ref[...] = scr[...].astype(BF16)

    return pl.pallas_call(
        body,
        out_shape=[
            jax.ShapeDtypeStruct((lines * cuts, LANES), BF16),
            jax.ShapeDtypeStruct((rows, 2), jnp.int32),
        ],
        scratch_shapes=[pltpu.VMEM((lines * cuts, LANES), F32)],
        compiler_params=params(20),
        cost_estimate=cost(2 * rows * lines * width, 4 * x.size),
    )(x, gain.reshape(1, width), routes)


def unpack(lines, width, groups, cap):
    cuts = width // LANES
    half = groups // 2

    def body(x_ref, *refs):
        outs, scr = refs[:-1], refs[-1]
        scr[...] = x_ref[...].astype(F32)

        @pl.loop(0, cuts)
        def _(c):
            cols = pl.ds(pl.multiple_of(c * LANES, LANES), LANES)
            for n, (first, count) in enumerate(SLOTS):
                for side in range(2):
                    for s in range(count):
                        start = side * half * cap * cuts + (first + s) * cuts + c
                        outs[2 * n + side][s * half : (s + 1) * half, cols] = scr[
                            pl.ds(start, half, stride=cap * cuts), :
                        ].astype(BF16)

    return pl.pallas_call(
        body,
        out_shape=[
            jax.ShapeDtypeStruct((half * count, width), BF16) for _, count in SLOTS for _ in range(2)
        ],
        scratch_shapes=[pltpu.VMEM(lines.shape, F32)],
        compiler_params=params(16),
        cost_estimate=cost(2e9, 4 * lines.size),
    )(lines)


def add_pack(owns, lefts, rights, count):
    part, width = owns[0].shape
    cuts = width // LANES
    half = part // count

    def body(*refs):
        o_ref, scr = refs[6:]

        @pl.loop(0, cuts)
        def _(c):
            cols = pl.ds(pl.multiple_of(c * LANES, LANES), LANES)
            for side in range(2):
                for s in range(count):
                    rows = slice(s * half, (s + 1) * half)
                    start = side * half * count * cuts + s * cuts + c
                    scr[pl.ds(start, half, stride=count * cuts), :] = sum(
                        refs[k + side][rows, cols].astype(F32) for k in (0, 2, 4)
                    )

        o_ref[...] = scr[...].astype(BF16)

    return pl.pallas_call(
        body,
        out_shape=jax.ShapeDtypeStruct((2 * part * cuts, LANES), BF16),
        scratch_shapes=[pltpu.VMEM((2 * part * cuts, LANES), F32)],
        compiler_params=params(),
        cost_estimate=cost(2e9, 16 * owns[0].size),
    )(*owns, *lefts, *rights)


def expert(blocks, w_gate, w_up, w_down, loops):
    part, width = blocks[0].shape
    number = len(blocks)
    units = w_gate.shape[1]
    steps = units // TILE
    rows = number * part // loops

    def body(*refs):
        ins, (g_ref, u_ref, d_ref) = refs[:number], refs[number : number + 3]
        outs, (x_scr, acc) = refs[number + 3 : 2 * number + 3], refs[2 * number + 3 :]
        step = pl.program_id(0)

        @pl.when(step == 0)
        def _():
            for n, ref in enumerate(ins):
                x_scr[n * part : (n + 1) * part, :] = ref[...]

        def block(at, first):
            x = x_scr[at, :]
            gate = jnp.dot(x, g_ref[...], preferred_element_type=F32)
            up = jnp.dot(x, u_ref[...], preferred_element_type=F32)
            hidden = (gate / (1.0 + jnp.exp(-gate)) * up).astype(BF16)
            out = jnp.dot(hidden, d_ref[...], preferred_element_type=F32)
            acc[at, :] = jnp.where(first, out, acc[at, :] + out)

        if loops == 1:
            block(slice(0, rows), step == 0)
        else:

            @pl.loop(0, loops)
            def _(i):
                block(pl.ds(pl.multiple_of(i * rows, rows), rows), step == 0)

        @pl.when(step == steps - 1)
        def _():
            for n, ref in enumerate(outs):
                ref[...] = acc[n * part : (n + 1) * part, :].astype(BF16)

    whole = pl.BlockSpec((part, width), lambda i: (0, 0))
    return pl.pallas_call(
        body,
        grid=(steps,),
        in_specs=[whole] * number
        + [
            pl.BlockSpec((width, TILE), lambda i: (0, i)),
            pl.BlockSpec((width, TILE), lambda i: (0, i)),
            pl.BlockSpec((TILE, width), lambda i: (i, 0)),
        ],
        out_specs=[whole] * number,
        out_shape=[jax.ShapeDtypeStruct((part, width), BF16)] * number,
        scratch_shapes=[
            pltpu.VMEM((number * part, width), BF16),
            pltpu.VMEM((number * part, width), F32),
        ],
        compiler_params=params(36),
        cost_estimate=cost(6 * number * part * width * units, 6 * width * units),
    )(*blocks, w_gate, w_up, w_down)


def add(one, two):
    def body(a_ref, b_ref, o_ref):
        o_ref[...] = (a_ref[...].astype(F32) + b_ref[...].astype(F32)).astype(BF16)

    return pl.pallas_call(
        body,
        out_shape=jax.ShapeDtypeStruct(one.shape, BF16),
        compiler_params=params(6),
        cost_estimate=cost(1e9, 6 * one.size),
    )(one, two)


def mix(ys, ws):
    rows, deep = ys[0].shape
    width = ws[0].shape[1]
    tile = 512

    def body(*refs):
        y_refs, w_refs, o_ref = refs[:4], refs[4:9], refs[9]
        total = sum(
            jnp.dot(y[...], w[...], preferred_element_type=F32)
            for y, w in zip(y_refs[:3], w_refs[:3])
        )
        for n in range(2):
            cols = slice(n * deep // 2, (n + 1) * deep // 2)
            total += jnp.dot(y_refs[3][:, cols], w_refs[3 + n][...], preferred_element_type=F32)
        o_ref[...] = total.astype(BF16)

    return pl.pallas_call(
        body,
        grid=(width // tile,),
        in_specs=[pl.BlockSpec(y.shape, lambda i: (0, 0)) for y in ys]
        + [pl.BlockSpec((w.shape[0], tile), lambda i: (0, i)) for w in ws],
        out_specs=pl.BlockSpec((rows, tile), lambda i: (0, i)),
        out_shape=jax.ShapeDtypeStruct((rows, width), BF16),
        compiler_params=params(),
        cost_estimate=cost(3e9, 6e6),
    )(*ys, *ws)


def combine(chunks, routes, slots, weight, experts, width):
    rows = routes.shape[0]
    cuts = width // LANES

    def body(*refs):
        ins, (r_ref, s_ref, w_ref, o_ref, scr, acc) = refs[: len(SLOTS)], refs[len(SLOTS) :]
        w0 = w_ref[:, 0:1]
        w1 = w_ref[:, 1:2]
        for n, ((first, count), x_ref) in enumerate(zip(SLOTS, ins)):
            lines = experts * count
            scr[0 : lines * cuts, :] = x_ref[...].astype(F32)
            col = lax.broadcasted_iota(jnp.int32, (rows, lines), 1)
            hot = []
            for k in range(2):
                r = r_ref[:, k : k + 1]
                s = s_ref[:, k : k + 1]
                d = jnp.where((s >= first) & (s < first + count), r * count + s - first, -1)
                hot.append(jnp.where(col == d, 1.0, 0.0).astype(BF16))
            both = jnp.concatenate(hot, axis=0)

            wide = cuts // 2

            @pl.loop(0, cuts // wide)
            def _(c):
                cols = pl.ds(pl.multiple_of(c * wide * LANES, wide * LANES), wide * LANES)
                part = jnp.concatenate(
                    [
                        scr[pl.ds(wide * c + i, lines, stride=cuts), :].astype(BF16)
                        for i in range(wide)
                    ],
                    axis=1,
                )
                got = jnp.dot(both, part, preferred_element_type=F32)
                term = w0 * got[:rows] + w1 * got[rows:]
                if n == 0:
                    acc[:, cols] = term
                else:
                    acc[:, cols] += term

        o_ref[...] = acc[...].astype(BF16)

    most = max(count for _, count in SLOTS)
    return pl.pallas_call(
        body,
        out_shape=jax.ShapeDtypeStruct((rows, width), BF16),
        scratch_shapes=[
            pltpu.VMEM((experts * most * cuts, LANES), F32),
            pltpu.VMEM((rows, width), F32),
        ],
        compiler_params=params(),
        cost_estimate=cost(4 * rows * experts * 5 * width, 4 * rows * width),
    )(*chunks, routes, slots, weight)


def retain(queries, keys, values, coarse, fine, decay_rate):
    span, wide = queries.shape
    heads = wide // DK
    half = DK // 2
    steps = coarse[0].shape[0]
    step = span // steps

    def body(r_ref, q_ref, k_ref, v_ref, cc_ref, cs_ref, fc_ref, fs_ref, y_ref, qd_ref, st_ref, q_scr, k_scr):
        lane = lax.broadcasted_iota(jnp.int32, (step, wide), 1)
        first = lane % DK < half
        sign = jnp.where(first, -1.0, 1.0)

        @pl.loop(0, steps)
        def _(n):
            rows = pl.ds(pl.multiple_of(n * step, step), step)
            c_cos = cc_ref[pl.ds(n, 1), :]
            c_sin = cs_ref[pl.ds(n, 1), :]
            cos = c_cos * fc_ref[...] - c_sin * fs_ref[...]
            sin = (c_sin * fc_ref[...] + c_cos * fs_ref[...]) * sign

            def turned(x):
                other = jnp.where(first, pltpu.roll(x, wide - half, 1), pltpu.roll(x, half, 1))
                return x * cos + other * sin

            q_scr[rows, :] = turned(q_ref[rows, :].astype(F32)) * DK ** (-0.5)
            k_scr[rows, :] = turned(k_ref[rows, :].astype(F32))

        i = lax.broadcasted_iota(jnp.int32, (QBLOCK, QBLOCK), 0)
        j = lax.broadcasted_iota(jnp.int32, (QBLOCK, QBLOCK), 1)
        diff = (i - j).astype(F32)
        at = lax.broadcasted_iota(jnp.int32, (QBLOCK, DK), 0).astype(F32)
        for h in range(heads):
            rate = r_ref[h]
            dmat = jnp.where(diff >= 0, jnp.exp(-rate * jnp.maximum(diff, 0.0)), 0.0)
            q_fall = jnp.exp(-rate * (at + 1.0))
            k_fall = jnp.exp(-rate * (QBLOCK - 1.0 - at))
            block_fall = jnp.exp(jnp.full((DK, DV), -rate * QBLOCK, F32))

            def block(b, state):
                rows = pl.ds(pl.multiple_of(b * QBLOCK, QBLOCK), QBLOCK)
                q = q_scr[rows, h * DK : (h + 1) * DK]
                k = k_scr[rows, h * DK : (h + 1) * DK]
                v = v_ref[rows, h * DV : (h + 1) * DV]
                scores = product(q, k, RIGHT) * dmat
                y_ref[rows, h * DV : (h + 1) * DV] = product(scores, v, PLAIN) + product(
                    q * q_fall, state, PLAIN
                )
                past = (b * QBLOCK).astype(F32)
                qd_ref[rows, h * DK : (h + 1) * DK] = q * jnp.exp(-rate * (at + (past + 1.0)))
                return state * block_fall + product(k * k_fall, v, LEFT)

            state = lax.fori_loop(0, span // QBLOCK, block, jnp.zeros((DK, DV), F32))
            st_ref[h * DK : (h + 1) * DK, :] = state

    return pl.pallas_call(
        body,
        in_specs=[pl.BlockSpec(memory_space=pltpu.SMEM)] + [pl.BlockSpec()] * 7,
        out_shape=[
            jax.ShapeDtypeStruct((span, heads * DV), F32),
            jax.ShapeDtypeStruct((span, wide), F32),
            jax.ShapeDtypeStruct((wide, DV), F32),
        ],
        scratch_shapes=[pltpu.VMEM((span, wide), F32), pltpu.VMEM((span, wide), F32)],
        compiler_params=params(),
        cost_estimate=cost(8e9, 4 * span * wide * 8),
    )(decay_rate, queries, keys, values, *coarse, *fine)


def falls(r_ref, heads, steps):
    return jnp.concatenate(
        [jnp.exp(jnp.full((DK, DV), -1.0, F32) * (r_ref[h] * steps)) for h in range(heads)], axis=0
    )


SMEM = pl.BlockSpec(memory_space=pltpu.SMEM)


def chip_state(end, other, rate, at):
    heads = rate.shape[0]

    def body(r_ref, at_ref, e_ref, o_ref, t_ref):
        late = at_ref[2] == 1
        first = jnp.where(late, o_ref[...], e_ref[...])
        last = jnp.where(late, e_ref[...], o_ref[...])
        t_ref[...] = first * falls(r_ref, heads, 1.0) + last

    return pl.pallas_call(
        body,
        in_specs=[SMEM, SMEM] + [pl.BlockSpec()] * 2,
        out_shape=jax.ShapeDtypeStruct(end.shape, F32),
        compiler_params=params(4),
    )(rate, at, end, other)


def ring_state(total, got, rate, at, n_c):
    heads = rate.shape[0]
    n_y = len(got) + 1

    def body(r_ref, at_ref, t_ref, *refs):
        y = at_ref[1]
        before = jnp.zeros(total.shape, F32)
        whole = t_ref[...] * falls(r_ref, heads, (n_c * (n_y - 1 - y)).astype(F32))
        for k in range(1, n_y):
            g = refs[k - 1][...]
            before += jnp.where(y >= k, g * falls(r_ref, heads, float(n_c * (k - 1))), 0.0)
            left = n_y - 1 - lax.rem(y - k + n_y, n_y)
            whole += g * falls(r_ref, heads, (n_c * left).astype(F32))
        refs[-2][...] = before
        refs[-1][...] = whole

    return pl.pallas_call(
        body,
        in_specs=[SMEM, SMEM] + [pl.BlockSpec()] * n_y,
        out_shape=[jax.ShapeDtypeStruct(total.shape, F32)] * 2,
        compiler_params=params(6),
    )(rate, at, total, *got)


def step_state(far, got, rate, spans):
    heads = rate.shape[0]

    def body(r_ref, f_ref, g_ref, o_ref):
        o_ref[...] = f_ref[...] + g_ref[...] * falls(r_ref, heads, float(spans))

    return pl.pallas_call(
        body,
        in_specs=[SMEM] + [pl.BlockSpec()] * 2,
        out_shape=jax.ShapeDtypeStruct(far.shape, F32),
        compiler_params=params(4),
    )(rate, far, got)


def finish(inner, q_fallen, other, before, far, got, gain, rate, at, spans, n_c, tensor):
    span, wide = inner.shape
    heads = wide // DV
    share = span // tensor

    def body(r_ref, at_ref, y_ref, q_ref, o_ref, b_ref, f_ref, l_ref, g_ref, *refs):
        outs, st = refs[:-1], refs[-1]
        y, c, me = (at_ref[n] for n in (1, 2, 3))
        past = f_ref[...] + l_ref[...] * falls(r_ref, heads, float(spans))
        past = b_ref[...] + past * falls(r_ref, heads, (n_c * y).astype(F32))
        st[...] = jnp.where(c == 1, o_ref[...], 0.0) + past * falls(r_ref, heads, c.astype(F32))
        for away, out in zip((0, 1, 3, 2), outs):
            block = lax.rem(me + away, tensor)
            rows = pl.ds(pl.multiple_of(block * share, share), share)
            for h in range(heads):
                cols = slice(h * DV, (h + 1) * DV)
                ret = y_ref[rows, cols] + product(
                    q_ref[rows, h * DK : (h + 1) * DK], st[h * DK : (h + 1) * DK, :], PLAIN
                )
                mean_sq = jnp.mean(ret * ret, axis=-1, keepdims=True)
                out[:, cols] = (ret * lax.rsqrt(mean_sq + EPS) * g_ref[:, cols]).astype(BF16)

    return pl.pallas_call(
        body,
        in_specs=[SMEM, SMEM] + [pl.BlockSpec()] * 7,
        out_shape=[jax.ShapeDtypeStruct((share, wide), BF16)] * tensor,
        scratch_shapes=[pltpu.VMEM((heads * DK, DV), F32)],
        compiler_params=params(),
        cost_estimate=cost(2e9, 8 * span * wide),
    )(rate, at, inner, q_fallen, other, before, far, got, gain.reshape(1, wide))


def program(
    queries,
    keys,
    values,
    decay_rate,
    ret_gain,
    w_out,
    moe_in,
    ffn_gain,
    routes,
    route_weight,
    expert_gate,
    expert_up,
    expert_down,
):
    tensor = lax.axis_size("tp")
    groups = lax.axis_size(EP)
    span = queries.shape[0]
    heads = decay_rate.shape[0]
    rows, width = moe_in.shape
    experts = groups
    cap = 5 * rows * routes.shape[1] // (4 * experts)
    cuts = width // LANES
    to_right = [(i, (i + 1) % tensor) for i in range(tensor)]
    to_left = [(i, (i - 1) % tensor) for i in range(tensor)]
    across = [(i, (i + 2) % tensor) for i in range(tensor)]
    me = lax.axis_index("tp").astype(jnp.int32)
    part = w_out.shape[0] // 2

    def send(x, to):
        return lax.ppermute(x, "tp", to)

    w_left = send(w_out, to_right)
    w_right = send(w_out, to_left)

    sent, slots = place(moe_in, ffn_gain, routes, experts, cap)
    w_gate = expert_gate[0]
    w_up = expert_up[0]
    w_down = expert_down[0]

    n_z, n_y, n_c = (lax.axis_size(axis) for axis in EP)
    place_of = [lax.axis_index(axis) for axis in EP]
    at = jnp.stack([*place_of, me]).astype(jnp.int32)
    rate = decay_rate * span
    step = 32
    here = lax.axis_index(EP) * span
    half = DK // 2
    inv_freq = ROPE_BASE ** (-jnp.arange(half, dtype=F32) / half)
    coarse = (here + step * jnp.arange(span // step)).astype(F32)
    count = coarse.shape[0]
    angle = jnp.concatenate([coarse, jnp.arange(step, dtype=F32)])[:, None] * inv_freq[None, :]
    cosine = jnp.concatenate([jnp.cos(angle)] * (2 * heads), axis=1)
    sine = jnp.concatenate([jnp.sin(angle)] * (2 * heads), axis=1)
    coarse = (cosine[:count], sine[:count])
    fine = (cosine[count:], sine[count:])
    inner, q_fallen, end = retain(queries, keys, values, coarse, fine, decay_rate)

    arrived = lax.all_to_all(
        sent.reshape(experts, cap * cuts, LANES), EP, split_axis=0, concat_axis=0, tiled=True
    )
    owns = unpack(arrived.reshape(-1, LANES), width, groups, cap)

    answers = []
    for n, (_, count) in enumerate(SLOTS):
        own_a, own_b = owns[2 * n : 2 * n + 2]
        left_a = send(own_a, to_right)
        right_b = send(own_b, to_left)
        left_b = send(own_b, to_right)
        right_a = send(own_a, to_left)
        far_a = send(left_a, to_right)
        far_b = send(right_b, to_left)
        o_a, o_b, l_a, l_b, r_a, r_b = expert(
            (own_a, own_b, left_a, left_b, right_a, right_b), w_gate, w_up, w_down, 2
        )
        f_a, f_b = expert((far_a, far_b), w_gate, w_up, w_down, 1)
        got_lb = send(r_b, to_right)
        got_ra = send(l_a, to_left)
        via_a = send(f_a, to_right)
        via_b = send(f_b, to_left)
        r_sum = add(r_a, via_a)
        l_sum = add(l_b, via_b)
        got_la = send(r_sum, to_right)
        got_rb = send(l_sum, to_left)
        packed = add_pack((o_a, o_b), (got_la, got_lb), (got_ra, got_rb), count)
        answers.append(
            lax.all_to_all(
                packed.reshape(experts, count * cuts, LANES),
                EP,
                split_axis=0,
                concat_axis=0,
                tiled=True,
            ).reshape(-1, LANES)
        )

    other = lax.ppermute(end, EP[2], [(i, (i + 1) % n_c) for i in range(n_c)])
    total = chip_state(end, other, rate, at)
    got = []
    for k in range(1, n_y):
        got.append(lax.ppermute(total, EP[1], [(i, (i + k) % n_y) for i in range(n_y)]))
    before, whole = ring_state(total, got, rate, at, n_c)
    far = lax.ppermute(whole, EP[0], [(i, i + 1) for i in range(n_z - 1)])
    k = 1
    while True:
        plane = lax.ppermute(far, EP[0], [(i, i + k) for i in range(n_z - k)])
        spans = n_c * n_y * k
        if 2 * k >= n_z:
            break
        far = step_state(far, plane, rate, spans)
        k *= 2
    y_own, y_r, y_l, y_f = finish(
        inner, q_fallen, other, before, far, plane, ret_gain, rate, at, spans, n_c, tensor
    )
    y_left = send(y_r, to_right)
    y_right = send(y_l, to_left)
    y_far = send(y_f, across)
    w_far_a = send(w_left[:part], to_right)
    w_far_b = send(w_right[part:], to_left)
    mix_out = mix(
        (y_own, y_left, y_right, y_far), (w_out, w_left, w_right, w_far_a, w_far_b)
    )
    moe_out = combine(answers, routes, slots, route_weight, experts, width)
    return (mix_out, moe_out)


def solution(mesh):
    split = Mesh(mesh.devices.reshape(8, 4, 2, mesh.shape["tp"]), ("ep_0", "ep_1", "ep_2", "tp"))
    in_specs = (
        P(EP, "tp"),
        P(EP, "tp"),
        P(EP, "tp"),
        P("tp"),
        P("tp"),
        P("tp", None),
        P(EP_TP, None),
        P(),
        P(EP_TP, None),
        P(EP_TP, None),
        P(EP, None, "tp"),
        P(EP, None, "tp"),
        P(EP, "tp", None),
    )
    out_specs = (P(EP_TP, None), P(EP_TP, None))
    return jax.shard_map(program, mesh=split, in_specs=in_specs, out_specs=out_specs, check_vma=False)
```

```python
import jax
import jax.numpy as jnp
from jax import lax
from jax.experimental import pallas as pl
from jax.experimental.pallas import tpu as pltpu
from jax.sharding import Mesh
from jax.sharding import PartitionSpec as P


DK = 64
DV = 128
LANES = 128
QBLOCK = 256
TILE = 256
LOOPS = 3
EP = ("ep_0", "ep_1", "ep_2")
EP_TP = ("ep_0", "ep_1", "ep_2", "tp")
SLOTS = ((0, 2), (2, 3))

EPS = 1e-06
ROPE_BASE = 10000.0
F32 = jnp.float32
BF16 = jnp.bfloat16


def params(mib=14):
    return pltpu.CompilerParams(vmem_limit_bytes=mib * 1024 * 1024)


def cost(flops, num_bytes):
    return pl.CostEstimate(flops=int(flops), bytes_accessed=int(num_bytes), transcendentals=0)


def split(x):
    high = x.astype(BF16)
    return high, (x - high.astype(F32)).astype(BF16)


def product(a, b, dims):
    def dot(x, y):
        return lax.dot_general(x, y, (dims, ((), ())), preferred_element_type=F32)

    a_high, a_low = split(a)
    if b.dtype == BF16:
        return dot(a_high, b) + dot(a_low, b)
    b_high, b_low = split(b)
    return dot(a_high, b_high) + (dot(a_high, b_low) + dot(a_low, b_high))


PLAIN = ((1,), (0,))
RIGHT = ((1,), (1,))
LEFT = ((0,), (0,))


def place(x, gain, routes, experts, cap):
    rows, width = x.shape
    cuts = width // LANES
    lines = experts * cap

    def body(x_ref, g_ref, r_ref, o_ref, slot_ref, scr, flat):
        xf = x_ref[...].astype(F32)
        normed = (
            xf * lax.rsqrt(jnp.mean(xf * xf, axis=-1, keepdims=True) + EPS) * g_ref[...]
        ).astype(BF16)
        r0 = r_ref[:, 0:1]
        r1 = r_ref[:, 1:2]
        ids = lax.broadcasted_iota(jnp.int32, (rows, experts), 1)
        h0 = r0 == ids
        h1 = r1 == ids
        hits = jnp.where(h0 | h1, 1.0, 0.0).astype(BF16)
        tri = jnp.where(
            lax.broadcasted_iota(jnp.int32, (rows, rows), 0)
            > lax.broadcasted_iota(jnp.int32, (rows, rows), 1),
            1.0,
            0.0,
        ).astype(BF16)
        before = jnp.dot(tri, hits, preferred_element_type=F32)
        s0 = jnp.sum(jnp.where(h0, before, 0.0), axis=1, keepdims=True).astype(jnp.int32)
        s1 = jnp.sum(jnp.where(h1, before, 0.0), axis=1, keepdims=True).astype(jnp.int32)
        slot_ref[:, 0:1] = s0
        slot_ref[:, 1:2] = s1
        col = lax.broadcasted_iota(jnp.int32, (rows, lines), 1)
        hot = (col == r0 * cap + s0) | (col == r1 * cap + s1)
        hot = jnp.where(hot, 1.0, 0.0).T.astype(BF16)
        flat[...] = jnp.dot(hot, normed, preferred_element_type=F32)

        @pl.loop(0, cuts // 4)
        def _(n):
            for i in range(4):
                c = 4 * n + i
                cols = pl.ds(pl.multiple_of(c * LANES, LANES), LANES)
                scr[pl.ds(c, lines, stride=cuts), :] = flat[:, cols]

        o_ref[...] = scr[...].astype(BF16)

    return pl.pallas_call(
        body,
        out_shape=[
            jax.ShapeDtypeStruct((lines * cuts, LANES), BF16),
            jax.ShapeDtypeStruct((rows, 2), jnp.int32),
        ],
        scratch_shapes=[pltpu.VMEM((lines * cuts, LANES), F32), pltpu.VMEM((lines, width), F32)],
        compiler_params=params(20),
        cost_estimate=cost(2 * rows * lines * width, 4 * x.size),
    )(x, gain.reshape(1, width), routes)


def unpack(lines, width, groups, cap):
    cuts = width // LANES
    half = groups // 2

    def body(x_ref, *refs):
        outs, scr = refs[:-1], refs[-1]
        scr[...] = x_ref[...].astype(F32)

        @pl.loop(0, cuts)
        def _(c):
            cols = pl.ds(pl.multiple_of(c * LANES, LANES), LANES)
            for n, (first, count) in enumerate(SLOTS):
                for side in range(2):
                    for s in range(count):
                        start = side * half * cap * cuts + (first + s) * cuts + c
                        row = (n * side * count + s) * half
                        outs[2 if n else side][row : row + half, cols] = scr[
                            pl.ds(start, half, stride=cap * cuts), :
                        ].astype(BF16)

    near, late = (count * half for _, count in SLOTS)
    return pl.pallas_call(
        body,
        out_shape=[jax.ShapeDtypeStruct((size, width), BF16) for size in (near, near, 2 * late)],
        scratch_shapes=[pltpu.VMEM(lines.shape, F32)],
        compiler_params=params(16),
        cost_estimate=cost(2e9, 4 * lines.size),
    )(lines)


def add_pack(terms, count):
    rows, width = terms[0][0].shape
    part = rows // 2
    cuts = width // LANES
    half = part // count
    sizes = [len(term) for term in terms]

    def body(*refs):
        o_ref, scr = refs[-2:]

        @pl.loop(0, cuts)
        def _(c):
            cols = pl.ds(pl.multiple_of(c * LANES, LANES), LANES)
            for side in range(2):
                for s in range(count):
                    total = 0.0
                    at = 0
                    for size in sizes:
                        row = s * half + (side * part if size == 1 else 0)
                        ref = refs[at + (side if size == 2 else 0)]
                        total = total + ref[row : row + half, cols].astype(F32)
                        at += size
                    start = side * half * count * cuts + s * cuts + c
                    scr[pl.ds(start, half, stride=count * cuts), :] = total

        o_ref[...] = scr[...].astype(BF16)

    return pl.pallas_call(
        body,
        out_shape=jax.ShapeDtypeStruct((rows * cuts, LANES), BF16),
        scratch_shapes=[pltpu.VMEM((rows * cuts, LANES), F32)],
        compiler_params=params(),
        cost_estimate=cost(2e9, 8 * rows * width),
    )(*[x for term in terms for x in term])


def expert(blocks, w_gate, w_up, w_down, loops, ranges):
    sizes = [block.shape[0] for block in blocks]
    width = blocks[0].shape[1]
    number = len(blocks)
    units = w_gate.shape[1]
    steps = units // TILE
    total = sum(sizes)
    rows = total // loops

    def body(*refs):
        ins, (g_ref, u_ref, d_ref) = refs[:number], refs[number : number + 3]
        outs, (x_scr, acc) = refs[number + 3 : -2], refs[-2:]
        step = pl.program_id(0)

        @pl.when(step == 0)
        def _():
            first = 0
            for size, ref in zip(sizes, ins):
                x_scr[first : first + size, :] = ref[...]
                first += size

        def block(at, first):
            x = x_scr[at, :]
            gate = jnp.dot(x, g_ref[...], preferred_element_type=F32)
            up = jnp.dot(x, u_ref[...], preferred_element_type=F32)
            hidden = (gate / (1.0 + jnp.exp(-gate)) * up).astype(BF16)
            out = jnp.dot(hidden, d_ref[...], preferred_element_type=F32)
            acc[at, :] = jnp.where(first, out, acc[at, :] + out)

        if loops == 1:
            block(slice(0, rows), step == 0)
        else:

            @pl.loop(0, loops)
            def _(i):
                block(pl.ds(pl.multiple_of(i * rows, rows), rows), step == 0)

        @pl.when(step == steps - 1)
        def _():
            for (low, high), ref in zip(ranges, outs):
                ref[...] = acc[low:high, :].astype(BF16)

    def whole(size):
        return pl.BlockSpec((size, width), lambda i: (0, 0))

    given = [high - low for low, high in ranges]
    return pl.pallas_call(
        body,
        grid=(steps,),
        in_specs=[whole(size) for size in sizes]
        + [
            pl.BlockSpec((width, TILE), lambda i: (0, i)),
            pl.BlockSpec((width, TILE), lambda i: (0, i)),
            pl.BlockSpec((TILE, width), lambda i: (i, 0)),
        ],
        out_specs=[whole(size) for size in given],
        out_shape=[jax.ShapeDtypeStruct((size, width), BF16) for size in given],
        scratch_shapes=[
            pltpu.VMEM((total, width), BF16),
            pltpu.VMEM((total, width), F32),
        ],
        compiler_params=params(36),
        cost_estimate=cost(6 * total * width * units, 6 * width * units),
    )(*blocks, w_gate, w_up, w_down)


def add(whole, term, first):
    rows = term.shape[0]

    def body(a_ref, b_ref, o_ref):
        if rows < whole.shape[0]:
            o_ref[...] = a_ref[...]
        at = slice(first, first + rows)
        o_ref[at, :] = (a_ref[at, :].astype(F32) + b_ref[...].astype(F32)).astype(BF16)

    return pl.pallas_call(
        body,
        out_shape=jax.ShapeDtypeStruct(whole.shape, BF16),
        compiler_params=params(6),
        cost_estimate=cost(1e9, 6 * whole.size),
    )(whole, term)


def mix(ys, ws):
    rows, deep = ys[0].shape
    width = ws[0].shape[1]
    tile = 512

    def body(*refs):
        y_refs, w_refs, o_ref = refs[:4], refs[4:9], refs[9]
        total = sum(
            jnp.dot(y[...], w[...], preferred_element_type=F32)
            for y, w in zip(y_refs[:3], w_refs[:3])
        )
        for n in range(2):
            cols = slice(n * deep // 2, (n + 1) * deep // 2)
            total += jnp.dot(y_refs[3][:, cols], w_refs[3 + n][...], preferred_element_type=F32)
        o_ref[...] = total.astype(BF16)

    return pl.pallas_call(
        body,
        grid=(width // tile,),
        in_specs=[pl.BlockSpec(y.shape, lambda i: (0, 0)) for y in ys]
        + [pl.BlockSpec((w.shape[0], tile), lambda i: (0, i)) for w in ws],
        out_specs=pl.BlockSpec((rows, tile), lambda i: (0, i)),
        out_shape=jax.ShapeDtypeStruct((rows, width), BF16),
        compiler_params=params(),
        cost_estimate=cost(3e9, 6e6),
    )(*ys, *ws)


def combine(chunks, routes, slots, weight, experts, width):
    rows = routes.shape[0]
    cuts = width // LANES

    def body(*refs):
        ins, (r_ref, s_ref, w_ref, o_ref, scr, acc) = refs[: len(SLOTS)], refs[len(SLOTS) :]
        w0 = w_ref[:, 0:1]
        w1 = w_ref[:, 1:2]
        for n, ((first, count), x_ref) in enumerate(zip(SLOTS, ins)):
            lines = experts * count
            scr[0 : lines * cuts, :] = x_ref[...].astype(F32)
            col = lax.broadcasted_iota(jnp.int32, (rows, lines), 1)
            hot = []
            for k in range(2):
                r = r_ref[:, k : k + 1]
                s = s_ref[:, k : k + 1]
                d = jnp.where((s >= first) & (s < first + count), r * count + s - first, -1)
                hot.append(jnp.where(col == d, 1.0, 0.0).astype(BF16))
            both = jnp.concatenate(hot, axis=0)

            wide = cuts // 4

            @pl.loop(0, cuts // wide)
            def _(c):
                cols = pl.ds(pl.multiple_of(c * wide * LANES, wide * LANES), wide * LANES)
                part = jnp.concatenate(
                    [
                        scr[pl.ds(wide * c + i, lines, stride=cuts), :].astype(BF16)
                        for i in range(wide)
                    ],
                    axis=1,
                )
                got = jnp.dot(both, part, preferred_element_type=F32)
                term = w0 * got[:rows] + w1 * got[rows:]
                if n == 0:
                    acc[:, cols] = term
                else:
                    acc[:, cols] += term

        o_ref[...] = acc[...].astype(BF16)

    most = max(count for _, count in SLOTS)
    return pl.pallas_call(
        body,
        out_shape=jax.ShapeDtypeStruct((rows, width), BF16),
        scratch_shapes=[
            pltpu.VMEM((experts * most * cuts, LANES), F32),
            pltpu.VMEM((rows, width), F32),
        ],
        compiler_params=params(),
        cost_estimate=cost(4 * rows * experts * 5 * width, 4 * rows * width),
    )(*chunks, routes, slots, weight)


def retain(queries, keys, values, coarse, fine, decay_rate):
    span, wide = queries.shape
    heads = wide // DK
    half = DK // 2
    steps = coarse[0].shape[0]
    step = span // steps

    def body(r_ref, q_ref, k_ref, v_ref, cc_ref, cs_ref, fc_ref, fs_ref, y_ref, qd_ref, st_ref, q_scr, k_scr):
        lane = lax.broadcasted_iota(jnp.int32, (step, wide), 1)
        first = lane % DK < half
        sign = jnp.where(first, -1.0, 1.0)

        @pl.loop(0, steps)
        def _(n):
            rows = pl.ds(pl.multiple_of(n * step, step), step)
            c_cos = cc_ref[pl.ds(n, 1), :]
            c_sin = cs_ref[pl.ds(n, 1), :]
            cos = c_cos * fc_ref[...] - c_sin * fs_ref[...]
            sin = (c_sin * fc_ref[...] + c_cos * fs_ref[...]) * sign

            def turned(x):
                other = jnp.where(first, pltpu.roll(x, wide - half, 1), pltpu.roll(x, half, 1))
                return x * cos + other * sin

            q_scr[rows, :] = turned(q_ref[rows, :].astype(F32)) * DK ** (-0.5)
            k_scr[rows, :] = turned(k_ref[rows, :].astype(F32))

        i = lax.broadcasted_iota(jnp.int32, (QBLOCK, QBLOCK), 0)
        j = lax.broadcasted_iota(jnp.int32, (QBLOCK, QBLOCK), 1)
        diff = (i - j).astype(F32)
        at = lax.broadcasted_iota(jnp.int32, (QBLOCK, DK), 0).astype(F32)
        for h in range(heads):
            rate = r_ref[h]
            dmat = jnp.where(diff >= 0, jnp.exp(-rate * jnp.maximum(diff, 0.0)), 0.0)
            q_fall = jnp.exp(-rate * (at + 1.0))
            k_fall = jnp.exp(-rate * (QBLOCK - 1.0 - at))
            block_fall = jnp.exp(jnp.full((DK, DV), -rate * QBLOCK, F32))

            def block(b, state):
                rows = pl.ds(pl.multiple_of(b * QBLOCK, QBLOCK), QBLOCK)
                q = q_scr[rows, h * DK : (h + 1) * DK]
                k = k_scr[rows, h * DK : (h + 1) * DK]
                v = v_ref[rows, h * DV : (h + 1) * DV]
                scores = product(q, k, RIGHT) * dmat
                y_ref[rows, h * DV : (h + 1) * DV] = product(scores, v, PLAIN) + product(
                    q * q_fall, state, PLAIN
                )
                past = (b * QBLOCK).astype(F32)
                qd_ref[rows, h * DK : (h + 1) * DK] = q * jnp.exp(-rate * (at + (past + 1.0)))
                return state * block_fall + product(k * k_fall, v, LEFT)

            state = lax.fori_loop(0, span // QBLOCK, block, jnp.zeros((DK, DV), F32))
            st_ref[h * DK : (h + 1) * DK, :] = state

    return pl.pallas_call(
        body,
        in_specs=[pl.BlockSpec(memory_space=pltpu.SMEM)] + [pl.BlockSpec()] * 7,
        out_shape=[
            jax.ShapeDtypeStruct((span, heads * DV), F32),
            jax.ShapeDtypeStruct((span, wide), F32),
            jax.ShapeDtypeStruct((wide, DV), F32),
        ],
        scratch_shapes=[pltpu.VMEM((span, wide), F32), pltpu.VMEM((span, wide), F32)],
        compiler_params=params(),
        cost_estimate=cost(8e9, 4 * span * wide * 8),
    )(decay_rate, queries, keys, values, *coarse, *fine)


def falls(r_ref, heads, steps):
    return jnp.concatenate(
        [jnp.exp(jnp.full((DK, DV), -1.0, F32) * (r_ref[h] * steps)) for h in range(heads)], axis=0
    )


SMEM = pl.BlockSpec(memory_space=pltpu.SMEM)


def chip_state(end, other, rate, at):
    heads = rate.shape[0]

    def body(r_ref, at_ref, e_ref, o_ref, t_ref):
        late = at_ref[2] == 1
        first = jnp.where(late, o_ref[...], e_ref[...])
        last = jnp.where(late, e_ref[...], o_ref[...])
        t_ref[...] = first * falls(r_ref, heads, 1.0) + last

    return pl.pallas_call(
        body,
        in_specs=[SMEM, SMEM] + [pl.BlockSpec()] * 2,
        out_shape=jax.ShapeDtypeStruct(end.shape, F32),
        compiler_params=params(4),
    )(rate, at, end, other)


def step_state(far, got, rate, spans):
    heads = rate.shape[0]

    def body(r_ref, f_ref, g_ref, o_ref):
        o_ref[...] = f_ref[...] + g_ref[...] * falls(r_ref, heads, float(spans))

    return pl.pallas_call(
        body,
        in_specs=[SMEM] + [pl.BlockSpec()] * 2,
        out_shape=jax.ShapeDtypeStruct(far.shape, F32),
        compiler_params=params(4),
    )(rate, far, got)


def finish(inner, q_fallen, other, far, got, gain, rate, at, spans, tensor):
    span, wide = inner.shape
    heads = wide // DV
    share = span // tensor

    def body(r_ref, at_ref, y_ref, q_ref, o_ref, f_ref, l_ref, g_ref, *refs):
        outs, st = refs[:-1], refs[-1]
        c = at_ref[2]
        me = at_ref[3]
        past = f_ref[...] + l_ref[...] * falls(r_ref, heads, float(spans))
        st[...] = jnp.where(c == 1, o_ref[...], 0.0) + past * falls(r_ref, heads, c.astype(F32))
        for away, out in zip((0, 1, 3, 2), outs):
            block = lax.rem(me + away, tensor)
            rows = pl.ds(pl.multiple_of(block * share, share), share)
            for h in range(heads):
                cols = slice(h * DV, (h + 1) * DV)
                ret = y_ref[rows, cols] + product(
                    q_ref[rows, h * DK : (h + 1) * DK], st[h * DK : (h + 1) * DK, :], PLAIN
                )
                mean_sq = jnp.mean(ret * ret, axis=-1, keepdims=True)
                out[:, cols] = (ret * lax.rsqrt(mean_sq + EPS) * g_ref[:, cols]).astype(BF16)

    return pl.pallas_call(
        body,
        in_specs=[SMEM, SMEM] + [pl.BlockSpec()] * 6,
        out_shape=[jax.ShapeDtypeStruct((share, wide), BF16)] * tensor,
        scratch_shapes=[pltpu.VMEM((heads * DK, DV), F32)],
        compiler_params=params(),
        cost_estimate=cost(2e9, 8 * span * wide),
    )(rate, at, inner, q_fallen, other, far, got, gain.reshape(1, wide))


def program(
    queries,
    keys,
    values,
    decay_rate,
    ret_gain,
    w_out,
    moe_in,
    ffn_gain,
    routes,
    route_weight,
    expert_gate,
    expert_up,
    expert_down,
):
    tensor = lax.axis_size("tp")
    groups = lax.axis_size(EP)
    span = queries.shape[0]
    heads = decay_rate.shape[0]
    rows, width = moe_in.shape
    experts = groups
    cap = 5 * rows * routes.shape[1] // (4 * experts)
    cuts = width // LANES
    to_right = [(i, (i + 1) % tensor) for i in range(tensor)]
    to_left = [(i, (i - 1) % tensor) for i in range(tensor)]
    across = [(i, (i + 2) % tensor) for i in range(tensor)]
    me = lax.axis_index("tp").astype(jnp.int32)
    w_half = w_out.shape[0] // 2

    def send(x, to):
        return lax.ppermute(x, "tp", to)

    w_left = send(w_out, to_right)
    w_right = send(w_out, to_left)

    sent, slots = place(moe_in, ffn_gain, routes, experts, cap)
    w_gate = expert_gate[0]
    w_up = expert_up[0]
    w_down = expert_down[0]

    n_z, n_y, n_c = (lax.axis_size(axis) for axis in EP)
    place_of = [lax.axis_index(axis) for axis in EP]
    at = jnp.stack([*place_of, me]).astype(jnp.int32)
    rate = decay_rate * span
    step = 32
    here = lax.axis_index(EP) * span
    half = DK // 2
    inv_freq = ROPE_BASE ** (-jnp.arange(half, dtype=F32) / half)
    coarse = (here + step * jnp.arange(span // step)).astype(F32)
    count = coarse.shape[0]
    angle = jnp.concatenate([coarse, jnp.arange(step, dtype=F32)])[:, None] * inv_freq[None, :]
    cosine = jnp.concatenate([jnp.cos(angle)] * (2 * heads), axis=1)
    sine = jnp.concatenate([jnp.sin(angle)] * (2 * heads), axis=1)
    coarse = (cosine[:count], sine[:count])
    fine = (cosine[count:], sine[count:])
    inner, q_fallen, end = retain(queries, keys, values, coarse, fine, decay_rate)

    arrived = lax.all_to_all(
        sent.reshape(experts, cap * cuts, LANES), EP, split_axis=0, concat_axis=0, tiled=True
    )
    owns = unpack(arrived.reshape(-1, LANES), width, groups, cap)

    answers = []
    for n, (_, count) in enumerate(SLOTS):
        last = n == len(SLOTS) - 1
        if last:
            own = owns[2]
            part = own.shape[0] // 2
            left = send(own, to_right)
            right = send(own, to_left)
            far_a = send(left[:part], to_right)
            far_b = send(right[part:], to_left)
            blocks = (own, left, right)
            ranges = [(0, 2), (2, 3), (3, 4), (4, 5), (5, 6)]
        else:
            own_a, own_b = owns[:2]
            part = own_a.shape[0]
            left_a = send(own_a, to_right)
            right_b = send(own_b, to_left)
            left_b = send(own_b, to_right)
            right_a = send(own_a, to_left)
            far_a = send(left_a, to_right)
            far_b = send(right_b, to_left)
            blocks = (own_a, own_b, left_a, left_b, right_a, right_b)
            ranges = [(0, 2), (2, 4), (4, 6)]
        ranges = [(low * part, high * part) for low, high in ranges]
        o_all, *parts = expert(blocks, w_gate, w_up, w_down, LOOPS, ranges)
        f_a, f_b = expert((far_a, far_b), w_gate, w_up, w_down, 1, [(0, part), (part, 2 * part)])
        via_a = send(f_a, to_right)
        via_b = send(f_b, to_left)
        if last:
            l_a, l_b, r_a, r_b = parts
            got_lb = [send(r_b, to_right)]
            got_ra = [send(l_a, to_left)]
        else:
            l_b, r_a = parts
            got_lb, got_ra = [], []
        r_sum = add(r_a, via_a, 0)
        l_sum = add(l_b, via_b, 0 if last else via_b.shape[0])
        got_l = [send(r_sum, to_right), *got_lb]
        got_r = [*got_ra, send(l_sum, to_left)]
        packed = add_pack(([o_all], got_l, got_r), count)
        answers.append(
            lax.all_to_all(
                packed.reshape(experts, count * cuts, LANES),
                EP,
                split_axis=0,
                concat_axis=0,
                tiled=True,
            ).reshape(-1, LANES)
        )

    other = lax.ppermute(end, EP[2], [(i, (i + 1) % n_c) for i in range(n_c)])
    total = chip_state(end, other, rate, at)
    chips = n_z * n_y

    def ahead(x, k):
        return lax.ppermute(x, EP[:2], [(i, i + k) for i in range(chips - k)])

    far = ahead(total, 1)
    k = 1
    while True:
        got = ahead(far, k)
        spans = n_c * k
        if 2 * k >= chips:
            break
        far = step_state(far, got, rate, spans)
        k *= 2
    y_own, y_r, y_l, y_f = finish(
        inner, q_fallen, other, far, got, ret_gain, rate, at, spans, tensor
    )
    y_left = send(y_r, to_right)
    y_right = send(y_l, to_left)
    y_far = send(y_f, across)
    w_halves = (w_left[:w_half], w_right[w_half:])
    w_far_a = send(w_halves[0], to_right)
    w_far_b = send(w_halves[1], to_left)
    mix_out = mix(
        (y_own, y_left, y_right, y_far), (w_out, w_left, w_right, w_far_a, w_far_b)
    )
    moe_out = combine(answers, routes, slots, route_weight, experts, width)
    return (mix_out, moe_out)


def solution(mesh):
    split = Mesh(mesh.devices.reshape(8, 4, 2, mesh.shape["tp"]), ("ep_0", "ep_1", "ep_2", "tp"))
    in_specs = (
        P(EP, "tp"),
        P(EP, "tp"),
        P(EP, "tp"),
        P("tp"),
        P("tp"),
        P("tp", None),
        P(EP_TP, None),
        P(),
        P(EP_TP, None),
        P(EP_TP, None),
        P(EP, None, "tp"),
        P(EP, None, "tp"),
        P(EP, "tp", None),
    )
    out_specs = (P(EP_TP, None), P(EP_TP, None))
    return jax.shard_map(program, mesh=split, in_specs=in_specs, out_specs=out_specs, check_vma=False)
```

```python
import jax
import jax.numpy as jnp
from jax import lax
from jax.experimental import pallas as pl
from jax.experimental.pallas import tpu as pltpu
from jax.sharding import Mesh
from jax.sharding import PartitionSpec as P


DK = 64
DV = 128
LANES = 128
QBLOCK = 256
TILE = 256
LOOPS = 3
EP = ("ep_0", "ep_1", "ep_2")
EP_TP = ("ep_0", "ep_1", "ep_2", "tp")
SLOTS = ((0, 2), (2, 3))

EPS = 1e-06
ROPE_BASE = 10000.0
F32 = jnp.float32
BF16 = jnp.bfloat16


def params(mib=14):
    return pltpu.CompilerParams(vmem_limit_bytes=mib * 1024 * 1024)


def cost(flops, num_bytes):
    return pl.CostEstimate(flops=int(flops), bytes_accessed=int(num_bytes), transcendentals=0)


def split(x):
    high = x.astype(BF16)
    return high, (x - high.astype(F32)).astype(BF16)


def product(a, b, dims):
    def dot(x, y):
        return lax.dot_general(x, y, (dims, ((), ())), preferred_element_type=F32)

    a_high, a_low = split(a)
    if b.dtype == BF16:
        return dot(a_high, b) + dot(a_low, b)
    b_high, b_low = split(b)
    return dot(a_high, b_high) + (dot(a_high, b_low) + dot(a_low, b_high))


PLAIN = ((1,), (0,))
RIGHT = ((1,), (1,))
LEFT = ((0,), (0,))


def place(x, gain, routes, experts, cap):
    rows, width = x.shape
    cuts = width // LANES
    lines = experts * cap

    def body(x_ref, g_ref, r_ref, o_ref, slot_ref, scr, flat):
        xf = x_ref[...].astype(F32)
        normed = (
            xf * lax.rsqrt(jnp.mean(xf * xf, axis=-1, keepdims=True) + EPS) * g_ref[...]
        ).astype(BF16)
        r0 = r_ref[:, 0:1]
        r1 = r_ref[:, 1:2]
        ids = lax.broadcasted_iota(jnp.int32, (rows, experts), 1)
        h0 = r0 == ids
        h1 = r1 == ids
        hits = jnp.where(h0 | h1, 1.0, 0.0).astype(BF16)
        tri = jnp.where(
            lax.broadcasted_iota(jnp.int32, (rows, rows), 0)
            > lax.broadcasted_iota(jnp.int32, (rows, rows), 1),
            1.0,
            0.0,
        ).astype(BF16)
        before = jnp.dot(tri, hits, preferred_element_type=F32)
        s0 = jnp.sum(jnp.where(h0, before, 0.0), axis=1, keepdims=True).astype(jnp.int32)
        s1 = jnp.sum(jnp.where(h1, before, 0.0), axis=1, keepdims=True).astype(jnp.int32)
        slot_ref[:, 0:1] = s0
        slot_ref[:, 1:2] = s1
        col = lax.broadcasted_iota(jnp.int32, (rows, lines), 1)
        hot = (col == r0 * cap + s0) | (col == r1 * cap + s1)
        hot = jnp.where(hot, 1.0, 0.0).T.astype(BF16)
        flat[...] = jnp.dot(hot, normed, preferred_element_type=F32)

        @pl.loop(0, cuts // 4)
        def _(n):
            for i in range(4):
                c = 4 * n + i
                cols = pl.ds(pl.multiple_of(c * LANES, LANES), LANES)
                scr[pl.ds(c, lines, stride=cuts), :] = flat[:, cols]

        o_ref[...] = scr[...].astype(BF16)

    return pl.pallas_call(
        body,
        out_shape=[
            jax.ShapeDtypeStruct((lines * cuts, LANES), BF16),
            jax.ShapeDtypeStruct((rows, 2), jnp.int32),
        ],
        scratch_shapes=[pltpu.VMEM((lines * cuts, LANES), F32), pltpu.VMEM((lines, width), F32)],
        compiler_params=params(20),
        cost_estimate=cost(2 * rows * lines * width, 4 * x.size),
    )(x, gain.reshape(1, width), routes)


def unpack(lines, width, groups, cap, n):
    cuts = width // LANES
    half = groups // 2
    first, count = SLOTS[n]
    apart = n < len(SLOTS) - 1

    def body(x_ref, *refs):
        outs, scr = refs[:-1], refs[-1]
        scr[...] = x_ref[...].astype(F32)

        @pl.loop(0, cuts)
        def _(c):
            cols = pl.ds(pl.multiple_of(c * LANES, LANES), LANES)
            for side in range(2):
                for s in range(count):
                    start = side * half * cap * cuts + (first + s) * cuts + c
                    out, row = (outs[side], s) if apart else (outs[0], side * count + s)
                    out[row * half : (row + 1) * half, cols] = scr[
                        pl.ds(start, half, stride=cap * cuts), :
                    ].astype(BF16)

    sizes = [count * half] * 2 if apart else [2 * count * half]
    return pl.pallas_call(
        body,
        out_shape=[jax.ShapeDtypeStruct((size, width), BF16) for size in sizes],
        scratch_shapes=[pltpu.VMEM(lines.shape, F32)],
        compiler_params=params(16),
        cost_estimate=cost(2e9, 4 * lines.size),
    )(lines)


def add_pack(terms, count):
    rows, width = terms[0][0].shape
    part = rows // 2
    cuts = width // LANES
    half = part // count
    sizes = [len(term) for term in terms]

    def body(*refs):
        o_ref, scr = refs[-2:]

        @pl.loop(0, cuts)
        def _(c):
            cols = pl.ds(pl.multiple_of(c * LANES, LANES), LANES)
            for side in range(2):
                for s in range(count):
                    total = 0.0
                    at = 0
                    for size in sizes:
                        row = s * half + (side * part if size == 1 else 0)
                        ref = refs[at + (side if size == 2 else 0)]
                        total = total + ref[row : row + half, cols].astype(F32)
                        at += size
                    start = side * half * count * cuts + s * cuts + c
                    scr[pl.ds(start, half, stride=count * cuts), :] = total

        o_ref[...] = scr[...].astype(BF16)

    return pl.pallas_call(
        body,
        out_shape=jax.ShapeDtypeStruct((rows * cuts, LANES), BF16),
        scratch_shapes=[pltpu.VMEM((rows * cuts, LANES), F32)],
        compiler_params=params(),
        cost_estimate=cost(2e9, 8 * rows * width),
    )(*[x for term in terms for x in term])


def expert(blocks, w_gate, w_up, w_down, loops, ranges):
    sizes = [block.shape[0] for block in blocks]
    width = blocks[0].shape[1]
    number = len(blocks)
    units = w_gate.shape[1]
    steps = units // TILE
    total = sum(sizes)
    rows = total // loops

    def body(*refs):
        ins, (g_ref, u_ref, d_ref) = refs[:number], refs[number : number + 3]
        outs, (x_scr, acc) = refs[number + 3 : -2], refs[-2:]
        step = pl.program_id(0)

        @pl.when(step == 0)
        def _():
            first = 0
            for size, ref in zip(sizes, ins):
                x_scr[first : first + size, :] = ref[...]
                first += size

        def block(at, first):
            x = x_scr[at, :]
            gate = jnp.dot(x, g_ref[...], preferred_element_type=F32)
            up = jnp.dot(x, u_ref[...], preferred_element_type=F32)
            hidden = (gate / (1.0 + jnp.exp(-gate)) * up).astype(BF16)
            out = jnp.dot(hidden, d_ref[...], preferred_element_type=F32)
            acc[at, :] = jnp.where(first, out, acc[at, :] + out)

        if loops == 1:
            block(slice(0, rows), step == 0)
        else:

            @pl.loop(0, loops)
            def _(i):
                block(pl.ds(pl.multiple_of(i * rows, rows), rows), step == 0)

        @pl.when(step == steps - 1)
        def _():
            for (low, high), ref in zip(ranges, outs):
                ref[...] = acc[low:high, :].astype(BF16)

    def whole(size):
        return pl.BlockSpec((size, width), lambda i: (0, 0))

    given = [high - low for low, high in ranges]
    return pl.pallas_call(
        body,
        grid=(steps,),
        in_specs=[whole(size) for size in sizes]
        + [
            pl.BlockSpec((width, TILE), lambda i: (0, i)),
            pl.BlockSpec((width, TILE), lambda i: (0, i)),
            pl.BlockSpec((TILE, width), lambda i: (i, 0)),
        ],
        out_specs=[whole(size) for size in given],
        out_shape=[jax.ShapeDtypeStruct((size, width), BF16) for size in given],
        scratch_shapes=[
            pltpu.VMEM((total, width), BF16),
            pltpu.VMEM((total, width), F32),
        ],
        compiler_params=params(36),
        cost_estimate=cost(6 * total * width * units, 6 * width * units),
    )(*blocks, w_gate, w_up, w_down)


def add(whole, term, first):
    rows = term.shape[0]
    others = [n for n in range(0, whole.shape[0], rows) if n != first]
    step = 32

    def body(a_ref, b_ref, o_ref):
        @pl.loop(0, rows // step)
        def _(n):
            row = pl.multiple_of(n * step, step)
            at = pl.ds(first + row, step)
            o_ref[at, :] = (
                a_ref[at, :].astype(F32) + b_ref[pl.ds(row, step), :].astype(F32)
            ).astype(BF16)
            for other in others:
                same = pl.ds(other + row, step)
                o_ref[same, :] = a_ref[same, :]

    return pl.pallas_call(
        body,
        out_shape=jax.ShapeDtypeStruct(whole.shape, BF16),
        compiler_params=params(6),
        cost_estimate=cost(1e9, 6 * whole.size),
    )(whole, term)


def mix(ys, ws):
    rows, deep = ys[0].shape
    width = ws[0].shape[1]
    tile = 512

    def body(*refs):
        y_refs, w_refs, o_ref = refs[:4], refs[4:9], refs[9]
        total = sum(
            jnp.dot(y[...], w[...], preferred_element_type=F32)
            for y, w in zip(y_refs[:3], w_refs[:3])
        )
        for n in range(2):
            cols = slice(n * deep // 2, (n + 1) * deep // 2)
            total += jnp.dot(y_refs[3][:, cols], w_refs[3 + n][...], preferred_element_type=F32)
        o_ref[...] = total.astype(BF16)

    return pl.pallas_call(
        body,
        grid=(width // tile,),
        in_specs=[pl.BlockSpec(y.shape, lambda i: (0, 0)) for y in ys]
        + [pl.BlockSpec((w.shape[0], tile), lambda i: (0, i)) for w in ws],
        out_specs=pl.BlockSpec((rows, tile), lambda i: (0, i)),
        out_shape=jax.ShapeDtypeStruct((rows, width), BF16),
        compiler_params=params(),
        cost_estimate=cost(3e9, 6e6),
    )(*ys, *ws)


def combine(chunks, routes, slots, weight, experts, width):
    rows = routes.shape[0]
    cuts = width // LANES

    def body(*refs):
        ins, (r_ref, s_ref, w_ref, o_ref, scr, acc) = refs[: len(SLOTS)], refs[len(SLOTS) :]
        w0 = w_ref[:, 0:1]
        w1 = w_ref[:, 1:2]
        for n, ((first, count), x_ref) in enumerate(zip(SLOTS, ins)):
            lines = experts * count
            scr[0 : lines * cuts, :] = x_ref[...].astype(F32)
            col = lax.broadcasted_iota(jnp.int32, (rows, lines), 1)
            hot = []
            for k in range(2):
                r = r_ref[:, k : k + 1]
                s = s_ref[:, k : k + 1]
                d = jnp.where((s >= first) & (s < first + count), r * count + s - first, -1)
                hot.append(jnp.where(col == d, 1.0, 0.0).astype(BF16))
            both = jnp.concatenate(hot, axis=0)

            wide = cuts // 4

            @pl.loop(0, cuts // wide)
            def _(c):
                cols = pl.ds(pl.multiple_of(c * wide * LANES, wide * LANES), wide * LANES)
                part = jnp.concatenate(
                    [
                        scr[pl.ds(wide * c + i, lines, stride=cuts), :].astype(BF16)
                        for i in range(wide)
                    ],
                    axis=1,
                )
                got = jnp.dot(both, part, preferred_element_type=F32)
                term = w0 * got[:rows] + w1 * got[rows:]
                if n == 0:
                    acc[:, cols] = term
                else:
                    acc[:, cols] += term

        o_ref[...] = acc[...].astype(BF16)

    most = max(count for _, count in SLOTS)
    return pl.pallas_call(
        body,
        out_shape=jax.ShapeDtypeStruct((rows, width), BF16),
        scratch_shapes=[
            pltpu.VMEM((experts * most * cuts, LANES), F32),
            pltpu.VMEM((rows, width), F32),
        ],
        compiler_params=params(),
        cost_estimate=cost(4 * rows * experts * 5 * width, 4 * rows * width),
    )(*chunks, routes, slots, weight)


def retain(queries, keys, values, coarse, fine, decay_rate):
    span, wide = queries.shape
    heads = wide // DK
    half = DK // 2
    steps = coarse[0].shape[0]
    step = span // steps

    def body(r_ref, q_ref, k_ref, v_ref, cc_ref, cs_ref, fc_ref, fs_ref, y_ref, qd_ref, st_ref, q_scr, k_scr):
        lane = lax.broadcasted_iota(jnp.int32, (step, wide), 1)
        first = lane % DK < half
        sign = jnp.where(first, -1.0, 1.0)

        @pl.loop(0, steps)
        def _(n):
            rows = pl.ds(pl.multiple_of(n * step, step), step)
            c_cos = cc_ref[pl.ds(n, 1), :]
            c_sin = cs_ref[pl.ds(n, 1), :]
            cos = c_cos * fc_ref[...] - c_sin * fs_ref[...]
            sin = (c_sin * fc_ref[...] + c_cos * fs_ref[...]) * sign

            def turned(x):
                other = jnp.where(first, pltpu.roll(x, wide - half, 1), pltpu.roll(x, half, 1))
                return x * cos + other * sin

            q_scr[rows, :] = turned(q_ref[rows, :].astype(F32)) * DK ** (-0.5)
            k_scr[rows, :] = turned(k_ref[rows, :].astype(F32))

        i = lax.broadcasted_iota(jnp.int32, (QBLOCK, QBLOCK), 0)
        j = lax.broadcasted_iota(jnp.int32, (QBLOCK, QBLOCK), 1)
        diff = (i - j).astype(F32)
        at = lax.broadcasted_iota(jnp.int32, (QBLOCK, DK), 0).astype(F32)
        for h in range(heads):
            rate = r_ref[h]
            dmat = jnp.where(diff >= 0, jnp.exp(-rate * jnp.maximum(diff, 0.0)), 0.0)
            q_fall = jnp.exp(-rate * (at + 1.0))
            k_fall = jnp.exp(-rate * (QBLOCK - 1.0 - at))
            block_fall = jnp.exp(jnp.full((DK, DV), -rate * QBLOCK, F32))

            def block(b, state):
                rows = pl.ds(pl.multiple_of(b * QBLOCK, QBLOCK), QBLOCK)
                q = q_scr[rows, h * DK : (h + 1) * DK]
                k = k_scr[rows, h * DK : (h + 1) * DK]
                v = v_ref[rows, h * DV : (h + 1) * DV]
                scores = product(q, k, RIGHT) * dmat
                y_ref[rows, h * DV : (h + 1) * DV] = product(scores, v, PLAIN) + product(
                    q * q_fall, state, PLAIN
                )
                past = (b * QBLOCK).astype(F32)
                qd_ref[rows, h * DK : (h + 1) * DK] = q * jnp.exp(-rate * (at + (past + 1.0)))
                return state * block_fall + product(k * k_fall, v, LEFT)

            state = lax.fori_loop(0, span // QBLOCK, block, jnp.zeros((DK, DV), F32))
            st_ref[h * DK : (h + 1) * DK, :] = state

    return pl.pallas_call(
        body,
        in_specs=[pl.BlockSpec(memory_space=pltpu.SMEM)] + [pl.BlockSpec()] * 7,
        out_shape=[
            jax.ShapeDtypeStruct((span, heads * DV), F32),
            jax.ShapeDtypeStruct((span, wide), F32),
            jax.ShapeDtypeStruct((wide, DV), F32),
        ],
        scratch_shapes=[pltpu.VMEM((span, wide), F32), pltpu.VMEM((span, wide), F32)],
        compiler_params=params(),
        cost_estimate=cost(8e9, 4 * span * wide * 8),
    )(decay_rate, queries, keys, values, *coarse, *fine)


def falls(r_ref, heads, steps):
    return jnp.concatenate(
        [jnp.exp(jnp.full((DK, DV), -1.0, F32) * (r_ref[h] * steps)) for h in range(heads)], axis=0
    )


SMEM = pl.BlockSpec(memory_space=pltpu.SMEM)


def chip_state(end, other, rate, at):
    heads = rate.shape[0]

    def body(r_ref, at_ref, e_ref, o_ref, t_ref):
        late = at_ref[2] == 1
        first = jnp.where(late, o_ref[...], e_ref[...])
        last = jnp.where(late, e_ref[...], o_ref[...])
        t_ref[...] = first * falls(r_ref, heads, 1.0) + last

    return pl.pallas_call(
        body,
        in_specs=[SMEM, SMEM] + [pl.BlockSpec()] * 2,
        out_shape=jax.ShapeDtypeStruct(end.shape, F32),
        compiler_params=params(4),
    )(rate, at, end, other)


def step_state(far, got, rate, spans):
    heads = rate.shape[0]

    def body(r_ref, f_ref, g_ref, o_ref):
        o_ref[...] = f_ref[...] + g_ref[...] * falls(r_ref, heads, float(spans))

    return pl.pallas_call(
        body,
        in_specs=[SMEM] + [pl.BlockSpec()] * 2,
        out_shape=jax.ShapeDtypeStruct(far.shape, F32),
        compiler_params=params(4),
    )(rate, far, got)


def finish(inner, q_fallen, other, far, got, gain, rate, at, spans, tensor):
    span, wide = inner.shape
    heads = wide // DV
    share = span // tensor

    def body(r_ref, at_ref, y_ref, q_ref, o_ref, f_ref, l_ref, g_ref, *refs):
        outs, st = refs[:-1], refs[-1]
        c = at_ref[2]
        me = at_ref[3]
        past = f_ref[...] + l_ref[...] * falls(r_ref, heads, float(spans))
        past = jnp.where(c == 1, o_ref[...], 0.0) + past * falls(r_ref, heads, c.astype(F32))
        st[...] = jnp.zeros((heads * DK, wide), F32)
        for h in range(heads):
            keys = slice(h * DK, (h + 1) * DK)
            st[keys, h * DV : (h + 1) * DV] = past[keys, :]
        high, low = split(st[...])
        for away, out in zip((0, 1, 3, 2), outs):
            block = lax.rem(me + away, tensor)
            rows = pl.ds(pl.multiple_of(block * share, share), share)
            q_high, q_low = split(q_ref[rows, :])
            terms = ((q_high, high), (q_high, low), (q_low, high))
            cross = sum(jnp.dot(a, b, preferred_element_type=F32) for a, b in terms)
            for h in range(heads):
                cols = slice(h * DV, (h + 1) * DV)
                ret = y_ref[rows, cols] + cross[:, cols]
                mean_sq = jnp.mean(ret * ret, axis=-1, keepdims=True)
                out[:, cols] = (ret * lax.rsqrt(mean_sq + EPS) * g_ref[:, cols]).astype(BF16)

    return pl.pallas_call(
        body,
        in_specs=[SMEM, SMEM] + [pl.BlockSpec()] * 6,
        out_shape=[jax.ShapeDtypeStruct((share, wide), BF16)] * tensor,
        scratch_shapes=[pltpu.VMEM((heads * DK, wide), F32)],
        compiler_params=params(),
        cost_estimate=cost(2e9, 8 * span * wide),
    )(rate, at, inner, q_fallen, other, far, got, gain.reshape(1, wide))


def program(
    queries,
    keys,
    values,
    decay_rate,
    ret_gain,
    w_out,
    moe_in,
    ffn_gain,
    routes,
    route_weight,
    expert_gate,
    expert_up,
    expert_down,
):
    tensor = lax.axis_size("tp")
    groups = lax.axis_size(EP)
    span = queries.shape[0]
    heads = decay_rate.shape[0]
    rows, width = moe_in.shape
    experts = groups
    cap = 5 * rows * routes.shape[1] // (4 * experts)
    cuts = width // LANES
    to_right = [(i, (i + 1) % tensor) for i in range(tensor)]
    to_left = [(i, (i - 1) % tensor) for i in range(tensor)]
    across = [(i, (i + 2) % tensor) for i in range(tensor)]
    me = lax.axis_index("tp").astype(jnp.int32)
    w_half = w_out.shape[0] // 2

    def send(x, to):
        return lax.ppermute(x, "tp", to)

    w_left = send(w_out, to_right)
    w_right = send(w_out, to_left)

    sent, slots = place(moe_in, ffn_gain, routes, experts, cap)
    w_gate = expert_gate[0]
    w_up = expert_up[0]
    w_down = expert_down[0]

    n_z, n_y, n_c = (lax.axis_size(axis) for axis in EP)
    place_of = [lax.axis_index(axis) for axis in EP]
    at = jnp.stack([*place_of, me]).astype(jnp.int32)
    rate = decay_rate * span
    step = 32
    here = lax.axis_index(EP) * span
    half = DK // 2
    inv_freq = ROPE_BASE ** (-jnp.arange(half, dtype=F32) / half)
    coarse = (here + step * jnp.arange(span // step)).astype(F32)
    count = coarse.shape[0]
    angle = jnp.concatenate([coarse, jnp.arange(step, dtype=F32)])[:, None] * inv_freq[None, :]
    cosine = jnp.concatenate([jnp.cos(angle)] * (2 * heads), axis=1)
    sine = jnp.concatenate([jnp.sin(angle)] * (2 * heads), axis=1)
    coarse = (cosine[:count], sine[:count])
    fine = (cosine[count:], sine[count:])
    inner, q_fallen, end = retain(queries, keys, values, coarse, fine, decay_rate)

    arrived = lax.all_to_all(
        sent.reshape(experts, cap * cuts, LANES), EP, split_axis=0, concat_axis=0, tiled=True
    )
    arrived = arrived.reshape(-1, LANES)
    owns = unpack(arrived, width, groups, cap, 0)
    owns += unpack(arrived, width, groups, cap, 1)

    answers = []
    for n, (_, count) in enumerate(SLOTS):
        last = n == len(SLOTS) - 1
        if last:
            own = owns[2]
            part = own.shape[0] // 2
            left = send(own, to_right)
            right = send(own, to_left)
            far_a = send(left[:part], to_right)
            far_b = send(right[part:], to_left)
            blocks = (own, left, right)
            ranges = [(0, 2), (2, 3), (3, 4), (4, 5), (5, 6)]
        else:
            own_a, own_b = owns[:2]
            part = own_a.shape[0]
            left_a = send(own_a, to_right)
            right_b = send(own_b, to_left)
            left_b = send(own_b, to_right)
            right_a = send(own_a, to_left)
            far_a = send(left_a, to_right)
            far_b = send(right_b, to_left)
            blocks = (own_a, own_b, left_a, left_b, right_a, right_b)
            ranges = [(0, 2), (2, 4), (4, 6)]
        ranges = [(low * part, high * part) for low, high in ranges]
        o_all, *parts = expert(blocks, w_gate, w_up, w_down, LOOPS, ranges)
        f_a, f_b = expert((far_a, far_b), w_gate, w_up, w_down, 1, [(0, part), (part, 2 * part)])
        via_a = send(f_a, to_right)
        via_b = send(f_b, to_left)
        if last:
            l_a, l_b, r_a, r_b = parts
            got_lb = [send(r_b, to_right)]
            got_ra = [send(l_a, to_left)]
        else:
            l_b, r_a = parts
            got_lb, got_ra = [], []
        r_sum = add(r_a, via_a, 0)
        l_sum = add(l_b, via_b, 0 if last else via_b.shape[0])
        got_l = [send(r_sum, to_right), *got_lb]
        got_r = [*got_ra, send(l_sum, to_left)]
        packed = add_pack(([o_all], got_l, got_r), count)
        answers.append(
            lax.all_to_all(
                packed.reshape(experts, count * cuts, LANES),
                EP,
                split_axis=0,
                concat_axis=0,
                tiled=True,
            ).reshape(-1, LANES)
        )

    other = lax.ppermute(end, EP[2], [(i, (i + 1) % n_c) for i in range(n_c)])
    total = chip_state(end, other, rate, at)
    chips = n_z * n_y

    def ahead(x, k):
        return lax.ppermute(x, EP[:2], [(i, i + k) for i in range(chips - k)])

    far = ahead(total, 1)
    k = 1
    while True:
        got = ahead(far, k)
        spans = n_c * k
        if 2 * k >= chips:
            break
        far = step_state(far, got, rate, spans)
        k *= 2
    y_own, y_r, y_l, y_f = finish(
        inner, q_fallen, other, far, got, ret_gain, rate, at, spans, tensor
    )
    y_left = send(y_r, to_right)
    y_right = send(y_l, to_left)
    y_far = send(y_f, across)
    w_halves = (w_left[:w_half], w_right[w_half:])
    w_far_a = send(w_halves[0], to_right)
    w_far_b = send(w_halves[1], to_left)
    mix_out = mix(
        (y_own, y_left, y_right, y_far), (w_out, w_left, w_right, w_far_a, w_far_b)
    )
    moe_out = combine(answers, routes, slots, route_weight, experts, width)
    return (mix_out, moe_out)


def solution(mesh):
    split = Mesh(mesh.devices.reshape(8, 4, 2, mesh.shape["tp"]), ("ep_0", "ep_1", "ep_2", "tp"))
    in_specs = (
        P(EP, "tp"),
        P(EP, "tp"),
        P(EP, "tp"),
        P("tp"),
        P("tp"),
        P("tp", None),
        P(EP_TP, None),
        P(),
        P(EP_TP, None),
        P(EP_TP, None),
        P(EP, None, "tp"),
        P(EP, None, "tp"),
        P(EP, "tp", None),
    )
    out_specs = (P(EP_TP, None), P(EP_TP, None))
    return jax.shard_map(program, mesh=split, in_specs=in_specs, out_specs=out_specs, check_vma=False)
```
